32 devices in a mesh: kv: 8 (over z, y), tp: 4 (over x, core).
Axes of the slice: x: 2, y: 2, z: 4, core: 2. Of those that a mesh axis runs over, the one named last changes fastest.
Arguments:
- tokens: bfloat16 [256, 4096], P(None, ('kv', 'tp')), may hold values from -60 to 60
- past_state: float32 [256, 16, 128, 128], P('kv', 'tp'), may hold values from -4 to 4
- pre_gain: float32 [4096], replicated, may hold values from 0.1 to 1.9
- pre_gate: bfloat16 [4096, 11264], P(None, ('kv', 'tp')), may hold values from -0.09375 to 0.09375
- pre_up: bfloat16 [4096, 11264], P(None, ('kv', 'tp')), may hold values from -0.09375 to 0.09375
- pre_down: bfloat16 [11264, 4096], P(('kv', 'tp')), may hold values from -0.109375 to 0.109375
- mix_gain: float32 [4096], replicated, may hold values from 0.1 to 1.9
- query_weight: bfloat16 [4096, 2048], P('kv', 'tp'), may hold values from -0.09375 to 0.09375
- forget_weight: bfloat16 [4096, 2048], P('kv', 'tp'), may hold values from -0.09375 to 0.09375
- value_weight: bfloat16 [4096, 2048], P('kv', 'tp'), may hold values from -0.09375 to 0.09375
- output_gate_weight: bfloat16 [4096, 2048], P('kv', 'tp'), may hold values from -0.09375 to 0.09375
- forget_floor: float32 [2048], P('tp'), may hold values from 0.02 to 0.9
- head_gain: float32 [128], replicated, may hold values from 0.1 to 1.9
- proj_out: bfloat16 [2048, 4096], P('tp', 'kv'), may hold values from -0.125 to 0.125
- post_gain: float32 [4096], replicated, may hold values from 0.1 to 1.9
- post_gate: bfloat16 [4096, 11264], P(None, ('kv', 'tp')), may hold values from -0.09375 to 0.09375
- post_up: bfloat16 [4096, 11264], P(None, ('kv', 'tp')), may hold values from -0.09375 to 0.09375
- post_down: bfloat16 [11264, 4096], P(('kv', 'tp')), may hold values from -0.109375 to 0.109375
Outputs:
- result: bfloat16 [256, 4096], P(None, ('kv', 'tp'))
- new_state: float32 [256, 16, 128, 128], P('kv', 'tp')
The draws below stay inside these ranges and needn't reach their ends.
All inputs are finite; a program needn't handle non-finite values.
Results may differ from the reference program's by a relative error of at most 0.014.
Values may be sent and summed in bfloat16 or wider, within the bound.
A program may use at most 128 MiB of HBM per device.

```python
import math
import jax
import jax.numpy as jnp
from jax import lax

D = 4096
FF = 11264
HEADS = 16
HEAD_DIM = 128
INNER = 2048
SEQS = 256
N_TP = 4


def draw_tokens(key, part):
    key_base = jax.random.fold_in(key, 11)
    key_rows = jax.random.fold_in(key, 12)
    key_cols = jax.random.fold_in(key, 13)
    column_pos = jnp.arange(D, dtype=jnp.float32) / D
    jitter = jax.random.uniform(key_cols, (1, D), jnp.float32, 0.7, 1.3)
    rising = 0.5 * jnp.exp(column_pos * jnp.log(4.0))
    row_scales = jnp.exp(jax.random.uniform(key_rows, (SEQS, 1), jnp.float32, jnp.log(0.5), jnp.log(5.0)))
    base_vals = jnp.clip(jax.random.normal(key_base, (SEQS, D), jnp.float32), -4.0, 4.0)
    return (base_vals * rising[None, :] * jitter * row_scales).astype(jnp.bfloat16)


def spiked(values, stream_key, source, target, parts, factor):
    def block_of(dim):
        return (jnp.arange(values.shape[dim]) // (values.shape[dim] // parts)).reshape((-1,) + (1,) * (values.ndim - 1 - dim))

    near = jax.random.permutation(stream_key, parts)[block_of(target)]
    second = (block_of(target) + parts // 2) % parts
    return jnp.where((block_of(source) == near) | (block_of(source) == second), factor * values, values)


def shard_levels(stream_key, dims, cuts, smallest, high):
    level, own = 1.0, jax.random.fold_in(stream_key, 6)
    for position, parts in cuts:
        steps = jnp.exp(jax.random.uniform(jax.random.fold_in(own, position), (parts,), jnp.float32, smallest / len(cuts), high / len(cuts)))
        level = level * jnp.repeat(steps, dims[position] // parts).reshape([-1 if axis == position else 1 for axis in range(len(dims))])
    return level


def scatter_about(rng, dims, scale, bound, split=(), kind=jnp.bfloat16):
    level = shard_levels(rng, dims, split, -0.22, 0.18) if split else 1.0
    values = jax.random.normal(rng, dims, jnp.float32) * scale * level
    return jnp.minimum(jnp.maximum(values, -bound), bound).astype(kind)


def bell_draw_with(own_key, extent, deviation, limit, cuts, heavy, kind=jnp.bfloat16):
    entries = deviation * jax.random.normal(own_key, extent, jnp.float32)
    if cuts:
        entries = entries * shard_levels(own_key, extent, cuts, -0.22, 0.18)
    return jnp.clip(spiked(entries, jax.random.fold_in(own_key, 3), *heavy), -limit, limit).astype(kind)


def setup_inputs(seed: int = 0) -> dict:
    keys = jax.random.split(jax.random.key(seed), 19)
    return {
        "tokens": draw_tokens(jax.random.fold_in(keys[18], 71), 0),
        "past_state": scatter_about(keys[1], (SEQS, HEADS, HEAD_DIM, HEAD_DIM), 0.3, 4.0, ((0, 8), (1, 4)), jnp.float32),
        "pre_gain": jnp.clip(1.0 + 0.18 * jax.random.normal(keys[2], (D,), jnp.float32), 0.1, 1.9),
        "pre_gate": scatter_about(keys[3], (D, FF), D ** -0.5, 0.09375, ((1, 32),)),
        "pre_up": scatter_about(keys[4], (D, FF), D ** -0.5, 0.09375, ((1, 32),)),
        "pre_down": bell_draw_with(keys[5], (FF, D), FF ** -0.5, 0.109375, ((0, 32),), (0, 1, 32, 2.75)),
        "mix_gain": jnp.clip(1.0 + 0.18 * jax.random.normal(keys[6], (D,), jnp.float32), 0.1, 1.9),
        "query_weight": scatter_about(keys[7], (D, INNER), D ** -0.5, 0.09375, ((0, 8), (1, 4))),
        "forget_weight": scatter_about(keys[8], (D, INNER), D ** -0.5, 0.09375, ((0, 8), (1, 4))),
        "value_weight": scatter_about(keys[9], (D, INNER), D ** -0.5, 0.09375, ((0, 8), (1, 4))),
        "output_gate_weight": scatter_about(keys[10], (D, INNER), D ** -0.5, 0.09375, ((0, 8), (1, 4))),
        "forget_floor": jnp.clip(jnp.exp(math.log(0.9) - 3.8066625 * jax.random.uniform(keys[11], (INNER,), jnp.float32) ** shard_levels(keys[11], (INNER,), ((0, 4),), -0.2, 0.2)), 0.02, 0.9),
        "head_gain": jnp.clip(1.0 + 0.18 * jax.random.normal(keys[12], (HEAD_DIM,), jnp.float32), 0.1, 1.9),
        "proj_out": scatter_about(keys[13], (INNER, D), INNER ** -0.5, 0.125, ((0, 4), (1, 8))),
        "post_gain": jnp.clip(1.0 + 0.18 * jax.random.normal(keys[14], (D,), jnp.float32), 0.1, 1.9),
        "post_gate": scatter_about(keys[15], (D, FF), D ** -0.5, 0.09375, ((1, 32),)),
        "post_up": scatter_about(keys[16], (D, FF), D ** -0.5, 0.09375, ((1, 32),)),
        "post_down": bell_draw_with(keys[17], (FF, D), FF ** -0.5, 0.109375, ((0, 32),), (0, 1, 32, 2.75)),
    }


epsilon = 1e-06

def half_step(activations, gain, w_gate, w_up, w_down):
    x_float = activations.astype(jnp.float32)
    row_scale = lax.rsqrt(lax.optimization_barrier(jnp.mean(x_float * x_float, axis=1, keepdims=True)) + epsilon)
    normed = (x_float * gain).astype(jnp.bfloat16)
    gate_pre = row_scale * jnp.dot(normed, w_gate, preferred_element_type=jnp.float32)
    up_pre = row_scale * jnp.dot(normed, w_up, preferred_element_type=jnp.float32)
    hidden = (jax.nn.silu(gate_pre) * up_pre).astype(jnp.bfloat16)
    down_out = jnp.dot(hidden, w_down, preferred_element_type=jnp.float32)
    return (x_float + 0.5 * down_out).astype(jnp.bfloat16)

def reference(tokens, past_state, pre_gain, pre_gate, pre_up, pre_down, mix_gain, query_weight, forget_weight, value_weight, output_gate_weight, forget_floor, head_gain, proj_out, post_gain, post_gate, post_up, post_down):
    after_first = half_step(tokens, pre_gain, pre_gate, pre_up, pre_down)
    first_float = after_first.astype(jnp.float32)
    row_scale = lax.rsqrt(lax.optimization_barrier(jnp.mean(first_float * first_float, axis=1, keepdims=True)) + epsilon)
    normed = (first_float * mix_gain).astype(jnp.bfloat16)
    row_count = tokens.shape[0]
    head_shape = (row_count, HEADS, HEAD_DIM)
    pre_query = row_scale * jnp.dot(normed, query_weight, preferred_element_type=jnp.float32)
    pre_forget = row_scale * jnp.dot(normed, forget_weight, preferred_element_type=jnp.float32)
    pre_value = row_scale * jnp.dot(normed, value_weight, preferred_element_type=jnp.float32)
    pre_gate_out = row_scale * jnp.dot(normed, output_gate_weight, preferred_element_type=jnp.float32)
    floors = forget_floor.reshape(HEADS, HEAD_DIM)
    forget_heads = pre_forget.reshape(head_shape)
    forget = floors + (1.0 - floors) * jax.nn.sigmoid(forget_heads)
    written = (1.0 - floors) * jax.nn.sigmoid(-forget_heads)
    query_act = jax.nn.silu(pre_query.reshape(head_shape))
    value_act = pre_value.reshape(head_shape)
    new_state = forget[:, :, :, None] * past_state + written[:, :, :, None] * value_act[:, :, None, :]
    readout = jnp.einsum('bhkv,bhk->bhv', new_state, query_act, precision=lax.Precision.HIGHEST)
    readout = readout * lax.rsqrt(lax.optimization_barrier(jnp.mean(readout * readout, axis=2, keepdims=True)) + epsilon) * head_gain
    mixed_in = (readout.reshape(row_count, INNER) * jax.nn.silu(pre_gate_out)).astype(jnp.bfloat16)
    per_group = INNER // N_TP
    total_sum = jnp.zeros((row_count, D), jnp.float32)
    for head_block in range(N_TP):
        lower = head_block * per_group
        partial_out = jnp.dot(mixed_in[:, lower:lower + per_group], proj_out[lower:lower + per_group], preferred_element_type=jnp.float32).astype(jnp.bfloat16)
        total_sum = total_sum + partial_out.astype(jnp.float32)
    second = (first_float + total_sum).astype(jnp.bfloat16)
    result = half_step(second, post_gain, post_gate, post_up, post_down)
    return (result, new_state)
```

```python
import functools

import jax
import jax.numpy as jnp
from jax import lax
from jax.experimental import pallas as pl
from jax.experimental.pallas import tpu as pltpu
from jax.sharding import PartitionSpec as P

D = 4096


epsilon = 1e-06


def half_inputs(activations, gain, w_gate, w_up):
    piece_float = lax.all_gather(activations, ("kv", "tp"), axis=1, tiled=True).astype(jnp.float32)
    normed = (piece_float * gain).astype(jnp.bfloat16)
    gate_acc = jnp.dot(normed, w_gate, preferred_element_type=jnp.float32)
    up_acc = jnp.dot(normed, w_up, preferred_element_type=jnp.float32)
    squares = jnp.sum(piece_float * piece_float, axis=1)
    row_scale = lax.rsqrt(squares / D + epsilon)[:, None]
    return (jax.nn.silu(row_scale * gate_acc) * (row_scale * up_acc)).astype(jnp.bfloat16)


def down_sum(hidden, w_down):
    return lax.psum_scatter(
        jnp.dot(hidden, w_down, preferred_element_type=jnp.float32),
        ("kv", "tp"),
        scatter_dimension=1,
        tiled=True,
    )


def per_device_plain(
    tokens,
    past_state,
    pre_gain,
    pre_gate,
    pre_up,
    pre_down,
    mix_gain,
    query_weight,
    forget_weight,
    value_weight,
    output_gate_weight,
    forget_floor,
    head_gain,
    proj_out,
    post_gain,
    post_gate,
    post_up,
    post_down,
):
    whole_rows = lax.all_gather(tokens, ("kv", "tp"), axis=1, tiled=True)
    whole_float = whole_rows.astype(jnp.float32)
    row_scale = lax.rsqrt(jnp.mean(whole_float * whole_float, axis=1, keepdims=True) + epsilon)
    normed = (whole_float * pre_gain).astype(jnp.bfloat16)
    gate_pre = row_scale * jnp.dot(normed, pre_gate, preferred_element_type=jnp.float32)
    up_pre = row_scale * jnp.dot(normed, pre_up, preferred_element_type=jnp.float32)
    hidden = (jax.nn.silu(gate_pre) * up_pre).astype(jnp.bfloat16)
    kv_sums = lax.psum_scatter(
        jnp.dot(hidden, pre_down, preferred_element_type=jnp.float32).astype(jnp.bfloat16),
        "kv",
        scatter_dimension=1,
        tiled=True,
    )
    block_sum = lax.psum(kv_sums, "tp").astype(jnp.float32)
    block_width = block_sum.shape[1]
    block_old = lax.dynamic_slice_in_dim(
        whole_rows, lax.axis_index("kv") * block_width, block_width, 1
    )
    block_rows = (block_old.astype(jnp.float32) + 0.5 * block_sum).astype(jnp.bfloat16)
    own_width = block_width // lax.axis_size("tp")
    after_first = lax.dynamic_slice_in_dim(
        block_rows, lax.axis_index("tp") * own_width, own_width, 1
    )
    block_width = block_rows.shape[1]
    block_float = block_rows.astype(jnp.float32)
    block_gain = lax.dynamic_slice_in_dim(
        mix_gain, lax.axis_index("kv") * block_width, block_width, 0
    )
    squares = lax.psum(jnp.sum(block_float * block_float, axis=1), "kv")
    normed = (block_float * block_gain).astype(jnp.bfloat16)
    own_rows = past_state.shape[0]
    weight_list = (query_weight, forget_weight, value_weight, output_gate_weight)
    projected = lax.psum_scatter(
        jnp.concatenate(
            [
                jnp.dot(normed, weight_part, preferred_element_type=jnp.float32)
                for weight_part in weight_list
            ],
            axis=1,
        ).astype(jnp.bfloat16),
        "kv",
        scatter_dimension=0,
        tiled=True,
    ).astype(jnp.float32)
    own_squares = lax.dynamic_slice_in_dim(squares, lax.axis_index("kv") * own_rows, own_rows, 0)
    projected = projected * lax.rsqrt(own_squares / D + epsilon)[:, None]
    pre_query, pre_forget, pre_value, pre_gate_out = jnp.split(projected, 4, axis=1)
    local_heads = past_state.shape[1]
    head_width = past_state.shape[2]
    head_shape = (own_rows, local_heads, head_width)
    floors = forget_floor.reshape(local_heads, head_width)
    forget_heads = pre_forget.reshape(head_shape)
    forget = floors + (1.0 - floors) * jax.nn.sigmoid(forget_heads)
    written = (1.0 - floors) * jax.nn.sigmoid(-forget_heads)
    query_act = jax.nn.silu(pre_query.reshape(head_shape))
    value_act = pre_value.reshape(head_shape)
    new_state = (
        forget[:, :, :, None] * past_state + written[:, :, :, None] * value_act[:, :, None, :]
    )
    readout = jnp.einsum("bhkv,bhk->bhv", new_state, query_act, precision=lax.Precision.HIGHEST)
    readout = (
        readout
        * lax.rsqrt(jnp.mean(readout * readout, axis=2, keepdims=True) + epsilon)
        * head_gain
    )
    mixed_in = (
        readout.reshape(own_rows, local_heads * head_width) * jax.nn.silu(pre_gate_out)
    ).astype(jnp.bfloat16)
    partials = jnp.dot(
        lax.all_gather(mixed_in, "kv", axis=0, tiled=True),
        proj_out,
        preferred_element_type=jnp.float32,
    ).astype(jnp.bfloat16)
    mixed_sum = lax.psum_scatter(partials, "tp", scatter_dimension=1, tiled=True).astype(
        jnp.float32
    )
    second = (after_first.astype(jnp.float32) + mixed_sum).astype(jnp.bfloat16)
    hidden_two = half_inputs(second, post_gain, post_gate, post_up)
    result = (second.astype(jnp.float32) + 0.5 * down_sum(hidden_two, post_down)).astype(
        jnp.bfloat16
    )
    return (result, new_state)


LANES = 128
LAST = (((1,), (1,)), ((), ()))
FIRST = (((0,), (0,)), ((), ()))
CORES, LINE, SIDE = 2, 4, 2
PLANE = SIDE * SIDE
F32, BF16 = jnp.float32, jnp.bfloat16
MESH = pl.DeviceIdType.MESH


class Grid:
    def __init__(self, n_kv, n_tp):
        self.nk, self.nt = n_kv, n_tp
        self.kv, self.tp = lax.axis_index("kv"), lax.axis_index("tp")
        self.z, self.y = self.kv // SIDE, self.kv % SIDE
        self.x, self.c = self.tp // CORES, self.tp % CORES
        self.oc = 1 - self.c
        y, x, c = self.y, self.x, self.c
        self.own = (y, x)
        self.a = (y + c * (1 - 2 * y), x + (1 - c) * (1 - 2 * x))
        self.b = (y + (1 - c) * (1 - 2 * y), x + c * (1 - 2 * x))
        self.diag = (1 - y, 1 - x)
        self.z1 = self.z + 1 - 2 * (self.z % 2)
        self.z3 = LINE - 1 - self.z
        self.z2 = LINE - 1 - self.z1
        self.mid = (self.z == 1) | (self.z == 2)

    def k(self, step):
        return lax.rem(self.kv + step, self.nk)

    def t(self, step):
        return lax.rem(self.tp + step, self.nt)

    def block(self, z, yx, c):
        return (z * SIDE + yx[0]) * self.nt + yx[1] * CORES + c

    def at(self, z, yx, c):
        return z * SIDE + yx[0], yx[1] * CORES + c


def remote(src, dst, send, recv, k, t):
    return pltpu.make_async_remote_copy(
        src_ref=src, dst_ref=dst, send_sem=send, recv_sem=recv,
        device_id={"kv": k, "tp": t}, device_id_type=MESH,
    )


class Sends:
    def __init__(self):
        self.started = []

    def start(self, copy, when=None):
        if when is None:
            copy.start()
        else:
            pl.when(when)(copy.start)
        self.started.append((copy, when))

    def finish(self):
        for copy, when in self.started:
            if when is None:
                copy.wait_send()
            else:
                pl.when(when)(copy.wait_send)


def barrier(g):
    sem = pltpu.get_barrier_semaphore()
    for step in range(1, g.nk):
        pl.semaphore_signal(sem, inc=1, device_id={"kv": g.k(step), "tp": g.tp}, device_id_type=MESH)
    for step in range(1, g.nt):
        pl.semaphore_signal(sem, inc=1, device_id={"kv": g.kv, "tp": g.t(step)}, device_id_type=MESH)
    pl.semaphore_wait(sem, g.nk - 1 + g.nt - 1)


def lanes(index, width=LANES):
    return pl.ds(pl.multiple_of(index * width, LANES), width)


def cols(ref, block, width=LANES):
    return ref.at[:, lanes(block, width)]


def ff_scratch(nk, nt, rows, depth, units):
    dma = pltpu.SemaphoreType.DMA
    blocks = nk * nt
    weights = [
        pltpu.VMEM((CORES * units, depth), BF16),
        pltpu.VMEM((CORES * units, depth // CORES), BF16),
        dma((2,)),
        dma((blocks // CORES,)),
        dma((blocks // CORES,)),
        dma((blocks // CORES,)),
    ]
    gather = [pltpu.VMEM((rows, depth), BF16), dma((blocks,)), dma((blocks,))]
    mid = [
        pltpu.VMEM((2 * units, rows), F32),
        pltpu.VMEM((rows, LANES), F32),
        pltpu.VMEM((CORES * units, rows), BF16),
        dma((1,)),
        dma((1,)),
    ]
    scatter = [
        pltpu.VMEM((LINE, rows, PLANE * LANES), F32),
        pltpu.VMEM((LINE, 2, rows, LANES), BF16),
        pltpu.VMEM((LINE, 2, rows, LANES), BF16),
        pltpu.VMEM((LINE, rows, LANES), BF16),
        pltpu.VMEM((LINE, rows, LANES), BF16),
        pltpu.VMEM((LINE - 1, rows, LANES), BF16),
        pltpu.VMEM((LINE - 1, rows, LANES), BF16),
        dma((LINE, 2)),
        dma((LINE, 2)),
        dma((LINE,)),
        dma((LINE,)),
        dma((LINE - 1,)),
        dma((LINE - 1,)),
    ]
    return weights + gather + mid + scatter


N_FF = 6 + 3 + 5 + 13


def load_weights(hbm, vmem, sem):
    copies = [pltpu.make_async_copy(a, b, sem.at[i]) for i, (a, b) in enumerate(zip(hbm, vmem))]
    for copy in copies:
        copy.start()
    return copies


class FeedForward:
    def __init__(self, g, gain, wg_h, wu_h, wd_h, scratch):
        self.g, self.gain, self.wd_h = g, gain, wd_h
        self.wgu, self.wd, self.gu_sem, self.wl, self.ws, self.wr = scratch[:6]
        self.full, self.send, self.recv = scratch[6:9]
        self.acc, self.sq, self.h2, self.hs, self.hr = scratch[9:14]
        self.scatter = scratch[14:]
        units = wg_h.shape[0]
        self.units = units
        self.gu_loads = [
            pltpu.make_async_copy(wg_h, self.wgu.at[pl.ds(0, units)], self.gu_sem.at[0]),
            pltpu.make_async_copy(wu_h, self.wgu.at[pl.ds(units, units)], self.gu_sem.at[1]),
        ]
        self.own_rows = pl.ds(pl.multiple_of(g.c * units, 16), units)

    def load_gate_up(self):
        for copy in self.gu_loads:
            copy.start()

    def down_local(self, q):
        src = cols(self.wd_h, q * CORES + self.g.c)
        return pltpu.make_async_copy(src, self.wd.at[self.own_rows, lanes(q)], self.wl.at[q])

    def down_remote(self, q):
        g = self.g
        src = cols(self.wd_h, q * CORES + g.oc)
        return remote(src, self.wd.at[self.own_rows, lanes(q)], self.ws.at[q], self.wr.at[q], g.kv, g.x * CORES + g.oc)

    def each(self, act):
        def body(q, carry):
            act(q)
            return carry

        lax.fori_loop(0, self.wd.shape[1] // LANES, body, 0)

    def load_down_own(self):
        self.each(lambda q: self.down_local(q).start())

    def send_down(self):
        self.each(lambda q: self.down_remote(q).start())

    def wait_down(self):
        def act(q):
            self.down_local(q).wait()
            self.down_remote(q).wait_recv()

        self.each(act)

    def gather(self, own_ref):
        g, full, recv = self.g, self.full, self.recv
        sends = Sends()

        def put(src, block, z, yx, c, when=None):
            k, t = g.at(z, yx, c)
            copy = remote(src, cols(full, block), self.send.at[len(sends.started)], recv.at[block], k, t)
            sends.start(copy, when)

        def arrived(block):
            remote(own_ref, cols(full, block), self.send.at[0], recv.at[block], g.kv, g.tp).wait_recv()

        def sibling(src, block):
            put(src, block, g.z, g.own, g.oc)

        def line(z, other):
            block = g.block(z, g.own, g.c)
            arrived(block)
            src = cols(full, block)
            put(src, block, g.z, g.b, g.c)
            put(src, block, g.z, g.a, g.c)
            if other is not None:
                put(src, block, other, g.own, g.c, g.mid)
            sibling(src, block)

        def from_a(z):
            block = g.block(z, g.a, g.c)
            arrived(block)
            put(cols(full, block), block, g.z, g.b, g.c)
            sibling(cols(full, block), block)

        def last(z, yx):
            block = g.block(z, yx, g.c)
            arrived(block)
            sibling(cols(full, block), block)

        half = PLANE * CORES * LANES // 2

        def product(z):
            for yy in range(SIDE):
                for xx in range(SIDE):
                    arrived(g.block(z, (yy, xx), g.oc))
            for part in range(2):
                at = lanes(z * 2 + part, half)
                x = full[:, at].astype(F32)
                u = (x * self.gain[:, at]).astype(BF16)
                self.acc[...] += lax.dot_general(self.wgu[:, at], u, LAST, preferred_element_type=F32)
                x2 = x * x
                total = self.sq[...]
                for i in range(half // LANES):
                    total = total + x2[:, i * LANES : (i + 1) * LANES]
                self.sq[...] = total

        mine = g.block(g.z, g.own, g.c)
        put(own_ref, mine, g.z1, g.own, g.c)
        put(own_ref, mine, g.z3, g.own, g.c)
        put(own_ref, mine, g.z, g.a, g.c)
        put(own_ref, mine, g.z, g.b, g.c)
        sibling(own_ref, mine)
        self.send_down()
        full[:, lanes(mine)] = own_ref[...]
        self.acc[...] = jnp.zeros_like(self.acc)
        self.sq[...] = jnp.zeros_like(self.sq)
        line(g.z1, g.z3)
        from_a(g.z)
        last(g.z, g.b)
        line(g.z3, g.z1)
        from_a(g.z1)
        last(g.z1, g.b)
        last(g.z, g.diag)
        line(g.z2, None)
        for copy in self.gu_loads:
            copy.wait()
        product(g.z)
        from_a(g.z3)
        last(g.z3, g.b)
        last(g.z1, g.diag)
        product(g.z1)
        from_a(g.z2)
        last(g.z2, g.b)
        last(g.z3, g.diag)
        last(g.z2, g.diag)
        product(g.z3)
        product(g.z2)
        return sends

    def hidden(self):
        g, units = self.g, self.units
        squares = jnp.sum(self.sq[...].T, axis=0, keepdims=True)
        scale = lax.rsqrt(squares / self.full.shape[1] + epsilon)
        gate, up = scale * self.acc[:units], scale * self.acc[units:]
        self.h2[self.own_rows] = (jax.nn.silu(gate) * up).astype(BF16)
        mine = self.h2.at[self.own_rows]
        copy = remote(mine, mine, self.hs.at[0], self.hr.at[0], g.kv, g.x * CORES + g.oc)
        copy.start()
        self.wait_down()
        copy.wait_recv()
        return copy

    def down(self, sends):
        g = self.g
        part, outb, inb, outa, ina, outz, inz, sb, rb, sa, ra, sz, rz = self.scatter
        order = (g.z2, g.z3, g.z1, g.z)
        width = PLANE * LANES

        def own_part(i, yx):
            return part[i, :, lanes(yx[0] * SIDE + yx[1])]

        def copy_b(i, j):
            k, t = g.at(g.z, g.b, g.c)
            return remote(outb.at[i, j], inb.at[i, j], sb.at[i, j], rb.at[i, j], k, t)

        def copy_a(i):
            k, t = g.at(g.z, g.a, g.c)
            return remote(outa.at[i], ina.at[i], sa.at[i], ra.at[i], k, t)

        def copy_z(i):
            k, t = g.at(order[i], g.own, g.c)
            return remote(outz.at[i], inz.at[i], sz.at[i], rz.at[i], k, t)

        def multiply(i):
            part[i] = lax.dot_general(self.h2[...], self.wd[:, lanes(order[i], width)], FIRST, preferred_element_type=F32)
            for j, yx in enumerate((g.diag, g.b)):
                outb[i, j] = own_part(i, yx).astype(BF16)
                sends.start(copy_b(i, j))

        def across_a(i):
            copy_b(i, 0).wait_recv()
            outa[i] = (own_part(i, g.a) + inb[i, 0].astype(F32)).astype(BF16)
            sends.start(copy_a(i))

        def total(i):
            copy_b(i, 1).wait_recv()
            copy_a(i).wait_recv()
            return own_part(i, g.own) + inb[i, 1].astype(F32) + ina[i].astype(F32)

        def along_z(i):
            outz[i] = total(i).astype(BF16)
            sends.start(copy_z(i))

        last = LINE - 1
        for i in range(LINE):
            multiply(i)
        across_a(0)
        for i in range(last):
            across_a(i + 1)
            along_z(i)
        out = total(last)
        for i in range(last):
            copy_z(i).wait_recv()
            out = out + inz[i].astype(F32)
        return out

    def run(self, own_ref):
        with jax.named_scope("gather"):
            sends = self.gather(own_ref)
        with jax.named_scope("hidden"):
            exchange = self.hidden()
        with jax.named_scope("down"):
            total = self.down(sends)
        sends.started.append((exchange, None))
        self.sends = sends
        return own_ref[...].astype(F32) + 0.5 * total

    def finish(self):
        self.sends.finish()
        self.each(lambda q: self.down_remote(q).wait_send())


def first_kernel(nk, nt, tok, gain, mgain, wg_h, wu_h, wd_h, q_h, f_h, v_h, o_h, first, projected, *scratch):
    g = Grid(nk, nt)
    ff, rest = scratch[:N_FF], scratch[N_FF:]
    mixw, mix_sem, block, bsend, brecv, normed, proj, mate_got, sums, got, sq, sq_got, msend, mrecv, psend, precv, qsend, qrecv = rest
    block_ff = FeedForward(g, gain, wg_h, wu_h, wd_h, ff)
    block_ff.load_gate_up()
    block_ff.load_down_own()
    mix_loads = load_weights((q_h, f_h, v_h, o_h), [mixw.at[i] for i in range(4)], mix_sem)
    barrier(g)
    first[...] = block_ff.run(tok).astype(BF16)

    copies = []
    for step in range(1, nt):
        copy = remote(first, cols(block, g.tp), bsend.at[step - 1], brecv.at[step - 1], g.kv, g.t(step))
        copy.start()
        copies.append(copy)
    block[:, pl.ds(pl.multiple_of(g.tp * LANES, LANES), LANES)] = first[...]
    for step in range(1, nt):
        src = g.t(nt - step)
        remote(first, cols(block, src), bsend.at[step - 1], brecv.at[step - 1], g.kv, src).wait_recv()
    width = block.shape[1]
    x = block[...].astype(F32)
    normed[...] = (x * mgain[:, pl.ds(pl.multiple_of(g.kv * width, LANES), width)]).astype(BF16)
    sq[...] = jnp.broadcast_to(jnp.sum(x * x, axis=1, keepdims=True), sq.shape)
    own_rows, inner = projected.shape[0], projected.shape[1] // 4

    def rows_of(k):
        return pl.ds(pl.multiple_of(k * own_rows, own_rows), own_rows)

    def q_copy(step):
        return remote(sq.at[rows_of(g.k(step))], sq_got.at[step - 1], qsend.at[step - 1], qrecv.at[step - 1], g.k(step), g.tp)

    nz, z, y = nk // 2, g.kv // 2, g.kv % 2

    def zi(dz):
        return lax.rem(z + dz, nz)

    def m_copy(i, dz):
        src = proj.at[i, zi(dz) * 2 + 1 - y]
        return remote(src, mate_got.at[i, dz], msend.at[i, dz], mrecv.at[i, dz], 2 * z + 1 - y, g.tp)

    def p_copy(i, dz):
        at = dz - 1
        return remote(sums.at[i, at], got.at[i, at], psend.at[i, at], precv.at[i, at], zi(dz) * 2 + y, g.tp)

    def mate_sum(i, dz):
        m_copy(i, dz).wait_recv()
        return proj[i, zi(dz) * 2 + y].astype(F32) + mate_got[i, dz].astype(F32)

    def forward(i):
        for dz in range(1, nz):
            sums[i, dz - 1] = mate_sum(i, dz).astype(BF16)
            p_copy(i, dz).start()

    for step in range(1, nk):
        q_copy(step).start()
    for i in range(4):
        mix_loads[i].wait()
        out = jnp.dot(normed[...], mixw[i], preferred_element_type=F32).astype(BF16)
        proj[i] = out.reshape(nk, own_rows, inner)
        for dz in range(1, nz + 1):
            m_copy(i, dz % nz).start()
        if i:
            forward(i - 1)
    forward(3)
    squares = sq[rows_of(g.kv), :]
    for step in range(1, nk):
        q_copy(step).wait_recv()
        squares = squares + sq_got[step - 1]
    scale = lax.rsqrt(squares[:, :1] / mgain.shape[1] + epsilon)
    for i in range(4):
        total = mate_sum(i, 0)
        for dz in range(1, nz):
            p_copy(i, dz).wait_recv()
            total = total + got[i, dz - 1].astype(F32)
        projected[:, i * inner : (i + 1) * inner] = total * scale
    block_ff.finish()
    for copy in copies:
        copy.wait_send()
    for step in range(1, nk):
        q_copy(step).wait_send()
    for i in range(4):
        for dz in range(nz):
            m_copy(i, dz).wait_send()
        for dz in range(1, nz):
            p_copy(i, dz).wait_send()


def recurrence_kernel(projected, past, floor, head_gain, new, mixed):
    rows, heads, width = past.shape[:3]
    inner = heads * width
    for h in range(heads):
        def part(i):
            return projected[:, i * inner + h * width : i * inner + (h + 1) * width]

        at = slice(h * width, (h + 1) * width)
        base = floor[:, at]
        forget = (base + (1.0 - base) * jax.nn.sigmoid(part(1))).T
        written = ((1.0 - base) * jax.nn.sigmoid(-part(1))).T
        query = jax.nn.silu(part(0)).T
        value = part(2)
        outs = []
        for n in range(rows):
            col = slice(n, n + 1)
            state = forget[:, col] * past[n, h] + written[:, col] * value[col]
            new[n, h] = state
            outs.append(jnp.sum(state * query[:, col], axis=0, keepdims=True))
        read = jnp.concatenate(outs, axis=0)
        read = read * lax.rsqrt(jnp.mean(read * read, axis=1, keepdims=True) + epsilon) * head_gain[...]
        mixed[:, at] = (read * jax.nn.silu(part(3))).astype(BF16)


def recurrence(projected, past_state, forget_floor, head_gain):
    rows, heads, width = past_state.shape[:3]
    inner, step = heads * width, 8
    state_spec = pl.BlockSpec((step, heads, width, width), lambda i: (i, 0, 0, 0))
    return pl.pallas_call(
        recurrence_kernel,
        grid=(rows // step,),
        out_shape=(
            jax.ShapeDtypeStruct(past_state.shape, F32),
            jax.ShapeDtypeStruct((rows, inner), BF16),
        ),
        in_specs=[
            pl.BlockSpec((step, 4 * inner), lambda i: (i, 0)),
            state_spec,
            pl.BlockSpec((1, inner), lambda i: (0, 0)),
            pl.BlockSpec((1, width), lambda i: (0, 0)),
        ],
        out_specs=(state_spec, pl.BlockSpec((step, inner), lambda i: (i, 0))),
        compiler_params=pltpu.CompilerParams(vmem_limit_bytes=32 * 1024 * 1024),
    )(projected, past_state, forget_floor[None], head_gain[None])


def second_kernel(nk, nt, y, first, gain, po_h, wg_h, wu_h, wd_h, result, *scratch):
    g = Grid(nk, nt)
    ff, rest = scratch[:N_FF], scratch[N_FF:]
    po, po_sem, yfull, ysend, yrecv, part, got, tsend, trecv, second = rest
    po_load = load_weights((po_h,), (po,), po_sem)
    block_ff = FeedForward(g, gain, wg_h, wu_h, wd_h, ff)
    block_ff.load_gate_up()
    block_ff.load_down_own()
    barrier(g)
    own_rows = y.shape[0]

    def rows_of(k):
        return pl.ds(pl.multiple_of(k * own_rows, own_rows), own_rows)

    def y_copy(step, k, src):
        return remote(y, yfull.at[rows_of(src)], ysend.at[step - 1], yrecv.at[step - 1], k, g.tp)

    for step in range(1, nk):
        y_copy(step, g.k(step), g.kv).start()
    yfull[rows_of(g.kv), :] = y[...]
    for step in range(1, nk):
        y_copy(step, g.k(step), g.k(nk - step)).wait_recv()
    po_load[0].wait()
    part[...] = jnp.dot(yfull[...], po[...], preferred_element_type=F32).astype(BF16)

    def t_copy(step):
        return remote(cols(part, g.t(step)), got.at[step - 1], tsend.at[step - 1], trecv.at[step - 1], g.kv, g.t(step))

    for step in range(1, nt):
        t_copy(step).start()
    total = part[:, pl.ds(pl.multiple_of(g.tp * LANES, LANES), LANES)].astype(F32)
    for step in range(1, nt):
        t_copy(step).wait_recv()
        total = total + got[step - 1].astype(F32)
    second[...] = (first[...].astype(F32) + total).astype(BF16)
    result[...] = block_ff.run(second).astype(BF16)
    block_ff.finish()
    for step in range(1, nk):
        y_copy(step, g.k(step), g.kv).wait_send()
    for step in range(1, nt):
        t_copy(step).wait_send()


def call(kernel, ident, outs, n_vmem, n_any, scratch, args):
    vmem, any_space = pl.BlockSpec(memory_space=pltpu.VMEM), pl.BlockSpec(memory_space=pl.ANY)
    return pl.pallas_call(
        kernel,
        out_shape=outs,
        in_specs=[vmem] * n_vmem + [any_space] * n_any,
        out_specs=jax.tree.map(lambda _: vmem, outs),
        scratch_shapes=scratch,
        compiler_params=pltpu.CompilerParams(
            collective_id=ident, has_side_effects=True, vmem_limit_bytes=56 * 1024 * 1024
        ),
    )(*args)


def per_device(
    tokens, past_state, pre_gain, pre_gate, pre_up, pre_down, mix_gain,
    query_weight, forget_weight, value_weight, output_gate_weight,
    forget_floor, head_gain, proj_out, post_gain, post_gate, post_up, post_down,
):
    nk, nt = lax.axis_size("kv"), lax.axis_size("tp")
    rows, depth, units = tokens.shape[0], pre_gate.shape[0], pre_gate.shape[1]
    own_rows, local_heads, head_width = past_state.shape[:3]
    inner = local_heads * head_width
    width = query_weight.shape[0]
    dma = pltpu.SemaphoreType.DMA
    base = ff_scratch(nk, nt, rows, depth, units)
    first, projected = call(
        functools.partial(first_kernel, nk, nt),
        0,
        (jax.ShapeDtypeStruct(tokens.shape, BF16), jax.ShapeDtypeStruct((own_rows, 4 * inner), F32)),
        3,
        7,
        base
        + [
            pltpu.VMEM((4, width, inner), BF16),
            dma((4,)),
            pltpu.VMEM((rows, width), BF16),
            dma((nt - 1,)),
            dma((nt - 1,)),
            pltpu.VMEM((rows, width), BF16),
            pltpu.VMEM((4, nk, own_rows, inner), BF16),
            pltpu.VMEM((4, nk // 2, own_rows, inner), BF16),
            pltpu.VMEM((4, nk // 2 - 1, own_rows, inner), BF16),
            pltpu.VMEM((4, nk // 2 - 1, own_rows, inner), BF16),
            pltpu.VMEM((rows, LANES), F32),
            pltpu.VMEM((nk - 1, own_rows, LANES), F32),
            dma((4, nk // 2)),
            dma((4, nk // 2)),
            dma((4, nk // 2 - 1)),
            dma((4, nk // 2 - 1)),
            dma((nk - 1,)),
            dma((nk - 1,)),
        ],
        (
            tokens, pre_gain[None], mix_gain[None], pre_gate.T, pre_up.T, pre_down,
            query_weight, forget_weight, value_weight, output_gate_weight,
        ),
    )
    new_state, mixed_in = recurrence(projected, past_state, forget_floor, head_gain)
    result = call(
        functools.partial(second_kernel, nk, nt),
        1,
        jax.ShapeDtypeStruct(tokens.shape, BF16),
        3,
        4,
        base
        + [
            pltpu.VMEM(proj_out.shape, BF16),
            dma((1,)),
            pltpu.VMEM((rows, inner), BF16),
            dma((nk - 1,)),
            dma((nk - 1,)),
            pltpu.VMEM((rows, width), BF16),
            pltpu.VMEM((nt - 1, rows, LANES), BF16),
            dma((nt - 1,)),
            dma((nt - 1,)),
            pltpu.VMEM((rows, LANES), BF16),
        ],
        (mixed_in, first, post_gain[None], proj_out, post_gate.T, post_up.T, post_down),
    )
    return (result, new_state)


def solution(mesh):
    placed = (
        P(None, ("kv", "tp")),
        P("kv", "tp", None, None),
        P(),
        P(None, ("kv", "tp")),
        P(None, ("kv", "tp")),
        P(("kv", "tp"), None),
        P(),
        P("kv", "tp"),
        P("kv", "tp"),
        P("kv", "tp"),
        P("kv", "tp"),
        P("tp"),
        P(),
        P("tp", "kv"),
        P(),
        P(None, ("kv", "tp")),
        P(None, ("kv", "tp")),
        P(("kv", "tp"), None),
    )
    blocks_fit = D == mesh.shape["kv"] * mesh.shape["tp"] * LANES and mesh.shape["tp"] == SIDE * CORES and mesh.shape["kv"] == LINE * SIDE
    return jax.shard_map(
        per_device if blocks_fit else per_device_plain,
        mesh=mesh,
        in_specs=placed,
        out_specs=(P(None, ("kv", "tp")), P("kv", "tp", None, None)),
        check_vma=False,
    )
```

```python
import functools

import jax
import jax.numpy as jnp
from jax import lax
from jax.experimental import pallas as pl
from jax.experimental.pallas import tpu as pltpu
from jax.sharding import PartitionSpec as P

D = 4096


epsilon = 1e-06


def half_inputs(activations, gain, w_gate, w_up):
    piece_float = lax.all_gather(activations, ("kv", "tp"), axis=1, tiled=True).astype(jnp.float32)
    normed = (piece_float * gain).astype(jnp.bfloat16)
    gate_acc = jnp.dot(normed, w_gate, preferred_element_type=jnp.float32)
    up_acc = jnp.dot(normed, w_up, preferred_element_type=jnp.float32)
    squares = jnp.sum(piece_float * piece_float, axis=1)
    row_scale = lax.rsqrt(squares / D + epsilon)[:, None]
    return (jax.nn.silu(row_scale * gate_acc) * (row_scale * up_acc)).astype(jnp.bfloat16)


def down_sum(hidden, w_down):
    return lax.psum_scatter(
        jnp.dot(hidden, w_down, preferred_element_type=jnp.float32),
        ("kv", "tp"),
        scatter_dimension=1,
        tiled=True,
    )


def per_device_plain(
    tokens,
    past_state,
    pre_gain,
    pre_gate,
    pre_up,
    pre_down,
    mix_gain,
    query_weight,
    forget_weight,
    value_weight,
    output_gate_weight,
    forget_floor,
    head_gain,
    proj_out,
    post_gain,
    post_gate,
    post_up,
    post_down,
):
    whole_rows = lax.all_gather(tokens, ("kv", "tp"), axis=1, tiled=True)
    whole_float = whole_rows.astype(jnp.float32)
    row_scale = lax.rsqrt(jnp.mean(whole_float * whole_float, axis=1, keepdims=True) + epsilon)
    normed = (whole_float * pre_gain).astype(jnp.bfloat16)
    gate_pre = row_scale * jnp.dot(normed, pre_gate, preferred_element_type=jnp.float32)
    up_pre = row_scale * jnp.dot(normed, pre_up, preferred_element_type=jnp.float32)
    hidden = (jax.nn.silu(gate_pre) * up_pre).astype(jnp.bfloat16)
    kv_sums = lax.psum_scatter(
        jnp.dot(hidden, pre_down, preferred_element_type=jnp.float32).astype(jnp.bfloat16),
        "kv",
        scatter_dimension=1,
        tiled=True,
    )
    block_sum = lax.psum(kv_sums, "tp").astype(jnp.float32)
    block_width = block_sum.shape[1]
    block_old = lax.dynamic_slice_in_dim(
        whole_rows, lax.axis_index("kv") * block_width, block_width, 1
    )
    block_rows = (block_old.astype(jnp.float32) + 0.5 * block_sum).astype(jnp.bfloat16)
    own_width = block_width // lax.axis_size("tp")
    after_first = lax.dynamic_slice_in_dim(
        block_rows, lax.axis_index("tp") * own_width, own_width, 1
    )
    block_width = block_rows.shape[1]
    block_float = block_rows.astype(jnp.float32)
    block_gain = lax.dynamic_slice_in_dim(
        mix_gain, lax.axis_index("kv") * block_width, block_width, 0
    )
    squares = lax.psum(jnp.sum(block_float * block_float, axis=1), "kv")
    normed = (block_float * block_gain).astype(jnp.bfloat16)
    own_rows = past_state.shape[0]
    weight_list = (query_weight, forget_weight, value_weight, output_gate_weight)
    projected = lax.psum_scatter(
        jnp.concatenate(
            [
                jnp.dot(normed, weight_part, preferred_element_type=jnp.float32)
                for weight_part in weight_list
            ],
            axis=1,
        ).astype(jnp.bfloat16),
        "kv",
        scatter_dimension=0,
        tiled=True,
    ).astype(jnp.float32)
    own_squares = lax.dynamic_slice_in_dim(squares, lax.axis_index("kv") * own_rows, own_rows, 0)
    projected = projected * lax.rsqrt(own_squares / D + epsilon)[:, None]
    pre_query, pre_forget, pre_value, pre_gate_out = jnp.split(projected, 4, axis=1)
    local_heads = past_state.shape[1]
    head_width = past_state.shape[2]
    head_shape = (own_rows, local_heads, head_width)
    floors = forget_floor.reshape(local_heads, head_width)
    forget_heads = pre_forget.reshape(head_shape)
    forget = floors + (1.0 - floors) * jax.nn.sigmoid(forget_heads)
    written = (1.0 - floors) * jax.nn.sigmoid(-forget_heads)
    query_act = jax.nn.silu(pre_query.reshape(head_shape))
    value_act = pre_value.reshape(head_shape)
    new_state = (
        forget[:, :, :, None] * past_state + written[:, :, :, None] * value_act[:, :, None, :]
    )
    readout = jnp.einsum("bhkv,bhk->bhv", new_state, query_act, precision=lax.Precision.HIGHEST)
    readout = (
        readout
        * lax.rsqrt(jnp.mean(readout * readout, axis=2, keepdims=True) + epsilon)
        * head_gain
    )
    mixed_in = (
        readout.reshape(own_rows, local_heads * head_width) * jax.nn.silu(pre_gate_out)
    ).astype(jnp.bfloat16)
    partials = jnp.dot(
        lax.all_gather(mixed_in, "kv", axis=0, tiled=True),
        proj_out,
        preferred_element_type=jnp.float32,
    ).astype(jnp.bfloat16)
    mixed_sum = lax.psum_scatter(partials, "tp", scatter_dimension=1, tiled=True).astype(
        jnp.float32
    )
    second = (after_first.astype(jnp.float32) + mixed_sum).astype(jnp.bfloat16)
    hidden_two = half_inputs(second, post_gain, post_gate, post_up)
    result = (second.astype(jnp.float32) + 0.5 * down_sum(hidden_two, post_down)).astype(
        jnp.bfloat16
    )
    return (result, new_state)


LANES = 128
LAST = (((1,), (1,)), ((), ()))
FIRST = (((0,), (0,)), ((), ()))
CORES, LINE, SIDE = 2, 4, 2
PLANE = SIDE * SIDE
F32, BF16 = jnp.float32, jnp.bfloat16
MESH = pl.DeviceIdType.MESH


class Grid:
    def __init__(self, n_kv, n_tp):
        self.nk, self.nt = n_kv, n_tp
        self.kv, self.tp = lax.axis_index("kv"), lax.axis_index("tp")
        self.z, self.y = self.kv // SIDE, self.kv % SIDE
        self.x, self.c = self.tp // CORES, self.tp % CORES
        self.oc = 1 - self.c
        y, x, c = self.y, self.x, self.c
        self.own = (y, x)
        self.a = (y + c * (1 - 2 * y), x + (1 - c) * (1 - 2 * x))
        self.b = (y + (1 - c) * (1 - 2 * y), x + c * (1 - 2 * x))
        self.diag = (1 - y, 1 - x)
        self.z1 = self.z + 1 - 2 * (self.z % 2)
        self.z3 = LINE - 1 - self.z
        self.z2 = LINE - 1 - self.z1
        self.mid = (self.z == 1) | (self.z == 2)

    def k(self, step):
        return lax.rem(self.kv + step, self.nk)

    def t(self, step):
        return lax.rem(self.tp + step, self.nt)

    def block(self, z, yx, c):
        return (z * SIDE + yx[0]) * self.nt + yx[1] * CORES + c

    def z_of(self, block):
        return block // self.nt

    def at(self, z, yx, c):
        return z * SIDE + yx[0], yx[1] * CORES + c


def remote(src, dst, send, recv, k, t):
    return pltpu.make_async_remote_copy(
        src_ref=src, dst_ref=dst, send_sem=send, recv_sem=recv,
        device_id={"kv": k, "tp": t}, device_id_type=MESH,
    )


def start(copy, when=None):
    if when is None:
        copy.start()
    else:
        pl.when(when)(copy.start)


def drain(ref, sem):
    pltpu.make_async_copy(ref, ref, sem).wait()


def greet(g):
    sem = pltpu.get_barrier_semaphore()
    for step in range(1, g.nk):
        pl.semaphore_signal(sem, inc=1, device_id={"kv": g.k(step), "tp": g.tp}, device_id_type=MESH)
    for step in range(1, g.nt):
        pl.semaphore_signal(sem, inc=1, device_id={"kv": g.kv, "tp": g.t(step)}, device_id_type=MESH)
    k, t = g.at(g.z, g.diag, g.c)
    pl.semaphore_signal(sem, inc=1, device_id={"kv": k, "tp": t}, device_id_type=MESH)


def barrier(g):
    pl.semaphore_wait(pltpu.get_barrier_semaphore(), g.nk - 1 + g.nt - 1 + 1)


def lanes(index, width=LANES):
    return pl.ds(pl.multiple_of(index * width, LANES), width)


def cols(ref, block, width=LANES):
    return ref.at[:, lanes(block, width)]


def ff_scratch(nk, nt, rows, depth, units):
    dma = pltpu.SemaphoreType.DMA
    blocks = nk * nt
    weights = [
        pltpu.VMEM((CORES * units, depth), BF16),
        pltpu.VMEM((CORES * units, depth // CORES), BF16),
        dma((2,)),
        dma((3,)),
    ]
    gather = [pltpu.VMEM((rows, depth), BF16), dma((3,)), dma((blocks // CORES,)), dma((blocks // CORES,)), dma((nk,))]
    mid = [
        pltpu.VMEM((2 * units, rows), F32),
        pltpu.VMEM((rows, LANES), F32),
        pltpu.VMEM((CORES * units, rows), BF16),
        dma((1,)),
        dma((1,)),
    ]
    scatter = [
        pltpu.VMEM((LINE, rows, PLANE * LANES), F32),
        pltpu.VMEM((LINE, 2, rows, LANES), BF16),
        pltpu.VMEM((LINE, 2, rows, LANES), BF16),
        pltpu.VMEM((LINE, rows, LANES), BF16),
        pltpu.VMEM((LINE, rows, LANES), BF16),
        pltpu.VMEM((LINE - 1, rows, LANES), BF16),
        pltpu.VMEM((LINE - 1, rows, LANES), BF16),
        dma((1,)),
        dma((LINE, 2)),
        dma((LINE,)),
        dma((LINE - 1,)),
    ]
    return weights + gather + mid + scatter


N_FF = 4 + 5 + 5 + 11


def load_weights(hbm, vmem, sem):
    copies = [pltpu.make_async_copy(a, b, sem.at[i]) for i, (a, b) in enumerate(zip(hbm, vmem))]
    for copy in copies:
        copy.start()
    return copies


class FeedForward:
    def __init__(self, g, gain, wg_h, wu_h, wd_h, scratch):
        self.g, self.gain, self.wd_h = g, gain, wd_h
        self.wgu, self.wd, self.gu_sem, self.wd_sem = scratch[:4]
        self.full, self.send, self.recv, self.recv_low, self.recv_core = scratch[4:9]
        self.acc, self.sq, self.h2, self.hs, self.hr = scratch[9:14]
        self.scatter = scratch[14:]
        units = wg_h.shape[0]
        self.units = units
        self.sent_down = False
        self.gu_loads = [
            pltpu.make_async_copy(wg_h, self.wgu.at[pl.ds(0, units)], self.gu_sem.at[0]),
            pltpu.make_async_copy(wu_h, self.wgu.at[pl.ds(units, units)], self.gu_sem.at[1]),
        ]
        self.own_rows = pl.ds(pl.multiple_of(g.c * units, 16), units)

    def load_gate_up(self):
        for copy in self.gu_loads:
            copy.start()

    def down_local(self, q):
        src = cols(self.wd_h, q * CORES + self.g.c)
        return pltpu.make_async_copy(src, self.wd.at[self.own_rows, lanes(q)], self.wd_sem.at[0])

    def down_remote(self, q):
        g = self.g
        src = cols(self.wd_h, q * CORES + g.oc)
        dst = self.wd.at[self.own_rows, lanes(q)]
        return remote(src, dst, self.wd_sem.at[1], self.wd_sem.at[2], g.kv, g.x * CORES + g.oc)

    def each(self, act):
        def body(q, carry):
            act(q)
            return carry

        lax.fori_loop(0, self.wd.shape[1] // LANES, body, 0)

    def load_down_own(self):
        self.each(lambda q: self.down_local(q).start())

    def send_down(self):
        self.sent_down = True
        self.each(lambda q: self.down_remote(q).start())

    def wait_down(self):
        drain(self.wd.at[self.own_rows], self.wd_sem.at[0])
        drain(self.wd.at[self.own_rows], self.wd_sem.at[2])

    def gather(self, own_ref):
        g, full = self.g, self.full
        rows = full.shape[0]
        cut = rows * 3 // 4
        whole, upper, lower = slice(0, rows), slice(0, cut), slice(cut, rows)
        sizes = (whole, upper, lower)
        always, inner = [0, 0, 0], [0, 0, 0]

        def put(src, block, at, z, yx, c, when=None):
            k, t = g.at(z, yx, c)
            dst = full.at[at, lanes(block)]
            kind = sizes.index(at)
            if c is g.oc:
                recv = self.recv_core.at[g.z_of(block)]
            else:
                recv = (self.recv_low if at is lower else self.recv).at[block // CORES]
            start(remote(dst if src is None else src, dst, self.send.at[kind], recv, k, t), when)
            (always if when is None else inner)[kind] += 1

        def arrived(block, at):
            drain(full.at[at, lanes(block)], (self.recv_low if at is lower else self.recv).at[block // CORES])

        def line(z, other):
            block = g.block(z, g.own, g.c)
            arrived(block, whole)
            if other is not None:
                put(None, block, whole, other, g.own, g.c, g.mid)
            else:
                put(None, block, upper, g.z, g.diag, g.c)
            put(None, block, upper, g.z, g.b, g.c)
            put(None, block, upper, g.z, g.a, g.c)
            put(None, block, whole, g.z, g.own, g.oc)

        def plane(yx):
            block = g.block(g.z, yx, g.c)
            arrived(block, whole)
            put(None, block, lower, g.z1, g.own, g.c)
            put(None, block, lower, g.z3, g.own, g.c)
            put(None, block, whole, g.z, g.own, g.oc)

        def from_a(z):
            block = g.block(z, g.a, g.c)
            arrived(block, upper)
            put(None, block, upper, g.z, g.b, g.c)
            put(None, block, upper, g.z, g.own, g.oc)

        def last(z, yx):
            block = g.block(z, yx, g.c)
            arrived(block, upper)
            put(None, block, upper, g.z, g.own, g.oc)

        def low(z, yx, other=None):
            block = g.block(z, yx, g.c)
            arrived(block, lower)
            if other is not None:
                put(None, block, lower, other, g.own, g.c, g.mid)
            put(None, block, lower, g.z, g.own, g.oc)

        half = SIDE * CORES * LANES

        def product(z, y):
            drain(full.at[:, lanes(z * SIDE + y, half // CORES)], self.recv_core.at[z * SIDE + y])
            at = lanes(z * SIDE + y, half)
            x = full[:, at].astype(F32)
            u = (x * self.gain[:, at]).astype(BF16)
            self.acc[...] += lax.dot_general(self.wgu[:, at], u, LAST, preferred_element_type=F32)
            x2 = x * x
            total = self.sq[...]
            for i in range(half // LANES):
                total = total + x2[:, i * LANES : (i + 1) * LANES]
            self.sq[...] = total

        oy = 1 - g.y
        mine = g.block(g.z, g.own, g.c)
        put(own_ref, mine, whole, g.z1, g.own, g.c)
        put(own_ref, mine, whole, g.z3, g.own, g.c)
        put(own_ref, mine, whole, g.z, g.a, g.c)
        put(own_ref, mine, whole, g.z, g.b, g.c)
        put(own_ref, mine, whole, g.z, g.diag, g.c)
        put(own_ref, mine, whole, g.z, g.own, g.oc)
        full[:, lanes(mine)] = own_ref[...]
        self.acc[...] = jnp.zeros_like(self.acc)
        self.sq[...] = jnp.zeros_like(self.sq)
        line(g.z1, g.z3)
        plane(g.a)
        plane(g.b)
        line(g.z3, g.z1)
        plane(g.diag)
        from_a(g.z1)
        last(g.z1, g.b)
        low(g.z1, g.a, g.z3)
        low(g.z1, g.b, g.z3)
        line(g.z2, None)
        if not self.sent_down:
            self.send_down()
        from_a(g.z3)
        last(g.z3, g.b)
        low(g.z3, g.a, g.z1)
        low(g.z3, g.b, g.z1)
        low(g.z1, g.diag, g.z3)
        last(g.z1, g.diag)
        for copy in self.gu_loads:
            copy.wait()
        product(g.z, g.y)
        low(g.z3, g.diag, g.z1)
        last(g.z3, g.diag)
        last(g.z2, g.a)
        last(g.z2, g.b)
        product(g.z, oy)
        product(g.z1, g.y)
        low(g.z2, g.a)
        low(g.z2, g.b)
        product(g.z1, oy)
        product(g.z3, g.y)
        last(g.z2, g.diag)
        low(g.z2, g.diag)
        product(g.z3, oy)
        product(g.z2, g.y)
        product(g.z2, oy)
        self.sent = list(zip(sizes, always, inner))

    def hidden(self):
        g, units = self.g, self.units
        squares = jnp.sum(self.sq[...].T, axis=0, keepdims=True)
        scale = lax.rsqrt(squares / self.full.shape[1] + epsilon)
        gate, up = scale * self.acc[:units], scale * self.acc[units:]
        self.h2[self.own_rows] = (jax.nn.silu(gate) * up).astype(BF16)
        mine = self.h2.at[self.own_rows]
        copy = remote(mine, mine, self.hs.at[0], self.hr.at[0], g.kv, g.x * CORES + g.oc)
        copy.start()
        self.wait_down()
        copy.wait_recv()
        return copy

    def down(self):
        g = self.g
        part, outb, inb, outa, ina, outz, inz, out_sem, rb, ra, rz = self.scatter
        sent = out_sem.at[0]
        order = (g.z2, g.z3, g.z1, g.z)
        width = PLANE * LANES

        def own_part(i, yx):
            return part[i, :, lanes(yx[0] * SIDE + yx[1])]

        def copy_b(i, j):
            k, t = g.at(g.z, g.b, g.c)
            return remote(outb.at[i, j], inb.at[i, j], sent, rb.at[i, j], k, t)

        def copy_a(i):
            k, t = g.at(g.z, g.a, g.c)
            return remote(outa.at[i], ina.at[i], sent, ra.at[i], k, t)

        def copy_z(i):
            k, t = g.at(order[i], g.own, g.c)
            return remote(outz.at[i], inz.at[i], sent, rz.at[i], k, t)

        def multiply(i):
            part[i] = lax.dot_general(self.h2[...], self.wd[:, lanes(order[i], width)], FIRST, preferred_element_type=F32)
            for j, yx in enumerate((g.diag, g.b)):
                outb[i, j] = own_part(i, yx).astype(BF16)
                copy_b(i, j).start()

        def across_a(i):
            copy_b(i, 0).wait_recv()
            outa[i] = (own_part(i, g.a) + inb[i, 0].astype(F32)).astype(BF16)
            copy_a(i).start()

        def total(i):
            copy_b(i, 1).wait_recv()
            copy_a(i).wait_recv()
            return own_part(i, g.own) + inb[i, 1].astype(F32) + ina[i].astype(F32)

        def along_z(i):
            outz[i] = total(i).astype(BF16)
            copy_z(i).start()

        last = LINE - 1
        for i in range(LINE):
            multiply(i)
        across_a(0)
        for i in range(last):
            across_a(i + 1)
            along_z(i)
        out = total(last)
        for i in range(last):
            copy_z(i).wait_recv()
            out = out + inz[i].astype(F32)
        return out

    def run(self, own_ref):
        with jax.named_scope("gather"):
            self.gather(own_ref)
        with jax.named_scope("hidden"):
            self.exchange = self.hidden()
        with jax.named_scope("down"):
            total = self.down()
        return own_ref[...].astype(F32) + 0.5 * total

    def finish(self):
        g, full = self.g, self.full
        self.exchange.wait_send()
        drain(self.wd.at[self.own_rows], self.wd_sem.at[1])
        drain(full.at[:, : (LINE * 4 - 1) * LANES], self.scatter[7].at[0])
        for kind, (rows, always, inner) in enumerate(self.sent):
            sem = self.send.at[kind]
            if inner:
                pl.when(g.mid)(lambda rows=rows, n=always + inner, sem=sem: drain(full.at[rows, : n * LANES], sem))
                pl.when(jnp.logical_not(g.mid))(lambda rows=rows, n=always, sem=sem: drain(full.at[rows, : n * LANES], sem))
            else:
                drain(full.at[rows, : always * LANES], sem)


def first_kernel(nk, nt, tok_h, gain_h, mgain_h, wg_h, wu_h, wd_h, q_h, f_h, v_h, o_h, first, projected, *scratch):
    g = Grid(nk, nt)
    greet(g)
    ff, rest = scratch[:N_FF], scratch[N_FF:]
    tok, gain, mgain, in_sem, mixw, mix_sem, block, bsend, brecv, normed, proj, ygot, outp, inp, outc, inc, sq, sq_got, sq_col, ys, yr, ps, pr, cs, cr, qsend, qrecv = rest
    in_loads = load_weights((tok_h, gain_h, mgain_h), (tok, gain, mgain), in_sem)
    block_ff = FeedForward(g, gain, wg_h, wu_h, wd_h, ff)
    block_ff.load_gate_up()
    block_ff.load_down_own()
    mix_loads = load_weights((q_h, f_h, v_h, o_h), [mixw.at[i] for i in range(4)], mix_sem)
    with jax.named_scope("barrier"):
        barrier(g)
        for copy in in_loads:
            copy.wait()
    first[...] = block_ff.run(tok).astype(BF16)

    rows, width = block.shape
    half = rows // 2
    far, near = 1 - g.z // 2, g.z // 2
    other = (1 - g.x) * CORES
    sib = g.x * CORES + g.oc

    def half_rows(q):
        return pl.ds(pl.multiple_of(q * half, half), half)

    def b_copy(src, index, q, t):
        dst = block.at[half_rows(q), lanes(index)]
        return remote(src, dst, bsend.at[0], brecv.at[index, q], g.kv, t)

    def b_wait(index, q):
        b_copy(first.at[half_rows(q)], index, q, sib).wait_recv()

    for q in (far, near):
        b_copy(first.at[half_rows(q)], g.tp, q, other + g.c).start()
        b_copy(first.at[half_rows(q)], g.tp, q, sib).start()
    block[:, lanes(g.tp)] = first[...]
    for q in (far, near):
        b_wait(other + g.c, q)
        b_copy(block.at[half_rows(q), lanes(other + g.c)], other + g.c, q, sib).start()
    own_rows, inner = projected.shape[0], projected.shape[1] // 4

    def normalise(q):
        b_wait(sib, q)
        b_wait(other + g.oc, q)
        x = block[half_rows(q), :].astype(F32)
        normed[half_rows(q), :] = (x * mgain[:, lanes(g.kv, width)]).astype(BF16)
        x2 = x * x
        squares = x2[:, :LANES]
        for i in range(1, width // LANES):
            squares = squares + x2[:, i * LANES : (i + 1) * LANES]
        sq[:, lanes(q, half)] = jnp.broadcast_to(jnp.sum(squares.T, axis=0, keepdims=True), (sq.shape[0], half))

    def rows_of(k):
        return pl.ds(pl.multiple_of(k * own_rows, own_rows), own_rows)

    def sq_part(k):
        return k * own_rows // LANES

    oy = 1 - g.y
    peers = ((g.z2, g.y), (g.z2, oy), (g.z3, g.y), (g.z3, oy), (g.z1, g.y), (g.z1, oy), (g.z, oy))

    def q_copy(i):
        k = peers[i][0] * SIDE + peers[i][1]
        return remote(cols(sq, sq_part(k)), sq_got.at[i], qsend.at[0], qrecv.at[0], k, g.tp)

    order = (g.z2, g.z3, g.z1, g.z)
    halves = 2
    wide = 4 * inner // halves

    def side(h):
        return slice(h * wide, (h + 1) * wide)

    def y_copy(j, h):
        src = proj.at[rows_of(order[j] * SIDE + 1 - g.y), pl.ds(h * wide, wide)]
        return remote(src, ygot.at[j, h], ys.at[0], yr.at[j, h], g.z * SIDE + 1 - g.y, g.tp)

    def p_copy(j, h):
        return remote(outp.at[j, h], inp.at[j, h], ps.at[0], pr.at[j, h], g.z1 * SIDE + g.y, g.tp)

    def c_copy(h):
        return remote(outc.at[h], inc.at[h], cs.at[0], cr.at[h], g.z3 * SIDE + g.y, g.tp)

    def y_sum(j, h):
        y_copy(j, h).wait_recv()
        return proj[rows_of(order[j] * SIDE + g.y), side(h)].astype(F32) + ygot[j, h].astype(F32)

    for copy in mix_loads:
        copy.wait()
    for part, q in enumerate((far, near)):
        with jax.named_scope("mixnorm"):
            normalise(q)
        for i in range(4) if part == 0 else range(4, nk - 1):
            q_copy(i).start()
        for h in range(halves):
            with jax.named_scope("mixdot"):
                for i in range(h * 2, h * 2 + 2):
                    out = jnp.dot(normed[half_rows(q), :], mixw[i], preferred_element_type=F32)
                    proj[half_rows(q), i * inner : (i + 1) * inner] = out.astype(BF16)
            y_copy(2 * part, h).start()
        for h in range(halves):
            y_copy(2 * part + 1, h).start()
    with jax.named_scope("mix0"):
        for h in range(halves):
            outp[0, h] = y_sum(0, h).astype(BF16)
            p_copy(0, h).start()
    with jax.named_scope("mix1"):
        for h in range(halves):
            total = y_sum(1, h)
            p_copy(0, h).wait_recv()
            outc[h] = (total + inp[0, h].astype(F32)).astype(BF16)
            c_copy(h).start()
    with jax.named_scope("mix2"):
        for h in range(halves):
            outp[1, h] = y_sum(2, h).astype(BF16)
            p_copy(1, h).start()
    with jax.named_scope("mix3"):
        squares = sq[:, lanes(sq_part(g.kv))]
        drain(sq_got, qrecv.at[0])
        for i in range(nk - 1):
            squares = squares + sq_got[i]
        sq_col[...] = jnp.broadcast_to(squares[:1], sq_col.shape).T
        mine = pl.ds(pl.multiple_of(g.kv * own_rows % LANES, own_rows), own_rows)
        scale = lax.rsqrt(sq_col[mine, :1] / mgain.shape[1] + epsilon)
        for h in range(halves):
            total = y_sum(3, h)
            p_copy(1, h).wait_recv()
            c_copy(h).wait_recv()
            projected[:, side(h)] = (total + inp[1, h].astype(F32) + inc[h].astype(F32)) * scale
    block_ff.finish()
    drain(block.at[:, : (nt - 1) * LANES], bsend.at[0])
    drain(ygot, ys.at[0])
    drain(outp, ps.at[0])
    drain(outc, cs.at[0])
    drain(sq_got, qsend.at[0])


def recurrence_kernel(projected, past, floor, head_gain, new, mixed, spread):
    rows, heads, width = past.shape[:3]
    inner = heads * width
    base = floor[...]
    forget = base + (1.0 - base) * jax.nn.sigmoid(projected[:, inner : 2 * inner])
    left = jnp.concatenate([forget, jax.nn.silu(projected[:, :inner])], axis=1)
    parts = []
    for _ in range(3):
        parts.append(left.astype(BF16).astype(F32))
        left = left - parts[-1]
    three = jnp.concatenate(parts, axis=0).astype(BF16)
    shape = (3 * rows, rows * width)
    chosen = lax.broadcasted_iota(jnp.int32, shape, 0) % rows == lax.broadcasted_iota(jnp.int32, shape, 1) // width
    spread[...] = lax.dot_general(three, chosen.astype(BF16), FIRST, preferred_element_type=F32)
    for h in range(heads):
        at = slice(h * width, (h + 1) * width)
        outs = []
        for n in range(rows):
            col = slice(n * width, (n + 1) * width)
            value = projected[n : n + 1, 2 * inner + h * width : 2 * inner + (h + 1) * width]
            state = value + spread[at, col] * (past[n, h] - value)
            new[n, h] = state
            query = spread[inner + h * width : inner + (h + 1) * width, col]
            outs.append(jnp.sum(state * query, axis=0, keepdims=True))
        read = jnp.concatenate(outs, axis=0)
        read = read * lax.rsqrt(jnp.mean(read * read, axis=1, keepdims=True) + epsilon) * head_gain[...]
        gate = projected[:, 3 * inner + h * width : 3 * inner + (h + 1) * width]
        mixed[:, at] = (read * jax.nn.silu(gate)).astype(BF16)


def recurrence(projected, past_state, forget_floor, head_gain):
    rows, heads, width = past_state.shape[:3]
    inner, step = heads * width, 8
    state_spec = pl.BlockSpec((step, heads, width, width), lambda i: (i, 0, 0, 0))
    return pl.pallas_call(
        recurrence_kernel,
        grid=(rows // step,),
        out_shape=(
            jax.ShapeDtypeStruct(past_state.shape, F32),
            jax.ShapeDtypeStruct((rows, inner), BF16),
        ),
        in_specs=[
            pl.BlockSpec((step, 4 * inner), lambda i: (i, 0)),
            state_spec,
            pl.BlockSpec((1, inner), lambda i: (0, 0)),
            pl.BlockSpec((1, width), lambda i: (0, 0)),
        ],
        out_specs=(state_spec, pl.BlockSpec((step, inner), lambda i: (i, 0))),
        scratch_shapes=[pltpu.VMEM((2 * inner, step * width), F32)],
        compiler_params=pltpu.CompilerParams(vmem_limit_bytes=32 * 1024 * 1024),
    )(projected, past_state, forget_floor[None], head_gain[None])


def second_kernel(nk, nt, y, first, gain, po_h, wg_h, wu_h, wd_h, result, *scratch):
    g = Grid(nk, nt)
    greet(g)
    ff, rest = scratch[:N_FF], scratch[N_FF:]
    po, po_sem, yfull, ysend, yrecv, part, got, tsend, trecv, second = rest
    po_load = load_weights((po_h,), (po,), po_sem)
    block_ff = FeedForward(g, gain, wg_h, wu_h, wd_h, ff)
    block_ff.load_gate_up()
    block_ff.load_down_own()
    with jax.named_scope("barrier"):
        barrier(g)
    own_rows = y.shape[0]
    oy = 1 - g.y

    def rows_of(k, count=1):
        return pl.ds(pl.multiple_of(k * own_rows * count, own_rows), own_rows * count)

    def put(src, owner, z, yy, when=None):
        start(remote(src, yfull.at[rows_of(owner)], ysend.at[0], yrecv.at[owner], z * SIDE + yy, g.tp), when)

    def arrived(owner):
        remote(y, yfull.at[rows_of(owner)], ysend.at[0], yrecv.at[owner], g.kv, g.tp).wait_recv()

    def line(z, other):
        owner = z * SIDE + g.y
        arrived(owner)
        src = yfull.at[rows_of(owner)]
        if other is not None:
            put(src, owner, other, g.y, g.mid)
        put(src, owner, g.z, oy)

    def t_copy(i, step):
        rows = rows_of(order[i], SIDE)
        return remote(
            part.at[rows, lanes(g.t(step))], got.at[step - 1, rows],
            tsend.at[0], trecv.at[0], g.kv, g.t(step),
        )

    order = (g.z, g.z1, g.z3, g.z2)

    def project(i):
        arrived(order[i] * SIDE + oy)
        rows = rows_of(order[i], SIDE)
        part[rows, :] = jnp.dot(yfull[rows, :], po[...], preferred_element_type=F32).astype(BF16)
        for step in range(1, nt):
            t_copy(i, step).start()

    with jax.named_scope("ygather"):
        put(y, g.kv, g.z1, g.y)
        put(y, g.kv, g.z3, g.y)
        put(y, g.kv, g.z, oy)
        yfull[rows_of(g.kv), :] = y[...]
        po_load[0].wait()
        line(g.z1, g.z3)
        line(g.z3, g.z1)
        project(0)
        line(g.z2, None)
        for i in range(1, LINE):
            project(i)
    with jax.named_scope("tscatter"):
        total = part[:, lanes(g.tp)].astype(F32)
        block_ff.send_down()
        drain(got, trecv.at[0])
        for step in range(1, nt):
            total = total + got[step - 1].astype(F32)
        second[...] = (first[...].astype(F32) + total).astype(BF16)
    result[...] = block_ff.run(second).astype(BF16)
    block_ff.finish()
    drain(got, tsend.at[0])
    pl.when(g.mid)(lambda: drain(yfull, ysend.at[0]))
    pl.when(jnp.logical_not(g.mid))(lambda: drain(yfull.at[: (nk - 2) * own_rows], ysend.at[0]))


def call(kernel, ident, outs, n_vmem, n_any, scratch, args):
    vmem, any_space = pl.BlockSpec(memory_space=pltpu.VMEM), pl.BlockSpec(memory_space=pl.ANY)
    return pl.pallas_call(
        kernel,
        out_shape=outs,
        in_specs=[vmem] * n_vmem + [any_space] * n_any,
        out_specs=jax.tree.map(lambda _: vmem, outs),
        scratch_shapes=scratch,
        cost_estimate=pl.CostEstimate(flops=50_000_000_000, bytes_accessed=1, transcendentals=0),
        compiler_params=pltpu.CompilerParams(
            collective_id=ident, has_side_effects=True, vmem_limit_bytes=34 * 1024 * 1024
        ),
    )(*args[:n_vmem], *[pltpu.with_memory_space_constraint(a, pltpu.HBM) for a in args[n_vmem:]])


def per_device(
    tokens, past_state, pre_gain, pre_gate, pre_up, pre_down, mix_gain,
    query_weight, forget_weight, value_weight, output_gate_weight,
    forget_floor, head_gain, proj_out, post_gain, post_gate, post_up, post_down,
):
    nk, nt = lax.axis_size("kv"), lax.axis_size("tp")
    rows, depth, units = tokens.shape[0], pre_gate.shape[0], pre_gate.shape[1]
    own_rows, local_heads, head_width = past_state.shape[:3]
    inner = local_heads * head_width
    width = query_weight.shape[0]
    dma = pltpu.SemaphoreType.DMA
    base = ff_scratch(nk, nt, rows, depth, units)
    first, projected = call(
        functools.partial(first_kernel, nk, nt),
        0,
        (jax.ShapeDtypeStruct(tokens.shape, BF16), jax.ShapeDtypeStruct((own_rows, 4 * inner), F32)),
        0,
        10,
        base
        + [
            pltpu.VMEM(tokens.shape, BF16),
            pltpu.VMEM((1, depth), F32),
            pltpu.VMEM((1, depth), F32),
            dma((3,)),
            pltpu.VMEM((4, width, inner), BF16),
            dma((4,)),
            pltpu.VMEM((rows, width), BF16),
            dma((1,)),
            dma((nt, 2)),
            pltpu.VMEM((rows, width), BF16),
            pltpu.VMEM((rows, 4 * inner), BF16),
            pltpu.VMEM((LINE, 2, own_rows, 2 * inner), BF16),
            pltpu.VMEM((2, 2, own_rows, 2 * inner), BF16),
            pltpu.VMEM((2, 2, own_rows, 2 * inner), BF16),
            pltpu.VMEM((2, own_rows, 2 * inner), BF16),
            pltpu.VMEM((2, own_rows, 2 * inner), BF16),
            pltpu.VMEM((8, rows), F32),
            pltpu.VMEM((nk - 1, 8, LANES), F32),
            pltpu.VMEM((LANES, LANES), F32),
            dma((1,)),
            dma((LINE, 2)),
            dma((1,)),
            dma((2, 2)),
            dma((1,)),
            dma((2,)),
            dma((1,)),
            dma((1,)),
        ],
        (
            tokens, pre_gain[None], mix_gain[None], pre_gate.T, pre_up.T, pre_down,
            query_weight, forget_weight, value_weight, output_gate_weight,
        ),
    )
    new_state, mixed_in = recurrence(projected, past_state, forget_floor, head_gain)
    result = call(
        functools.partial(second_kernel, nk, nt),
        1,
        jax.ShapeDtypeStruct(tokens.shape, BF16),
        3,
        4,
        base
        + [
            pltpu.VMEM(proj_out.shape, BF16),
            dma((1,)),
            pltpu.VMEM((rows, inner), BF16),
            dma((1,)),
            dma((nk,)),
            pltpu.VMEM((rows, width), BF16),
            pltpu.VMEM((nt - 1, rows, LANES), BF16),
            dma((1,)),
            dma((1,)),
            pltpu.VMEM((rows, LANES), BF16),
        ],
        (mixed_in, first, post_gain[None], proj_out, post_gate.T, post_up.T, post_down),
    )
    return (result, new_state)


def solution(mesh):
    placed = (
        P(None, ("kv", "tp")),
        P("kv", "tp", None, None),
        P(),
        P(None, ("kv", "tp")),
        P(None, ("kv", "tp")),
        P(("kv", "tp"), None),
        P(),
        P("kv", "tp"),
        P("kv", "tp"),
        P("kv", "tp"),
        P("kv", "tp"),
        P("tp"),
        P(),
        P("tp", "kv"),
        P(),
        P(None, ("kv", "tp")),
        P(None, ("kv", "tp")),
        P(("kv", "tp"), None),
    )
    blocks_fit = D == mesh.shape["kv"] * mesh.shape["tp"] * LANES and mesh.shape["tp"] == SIDE * CORES and mesh.shape["kv"] == LINE * SIDE
    return jax.shard_map(
        per_device if blocks_fit else per_device_plain,
        mesh=mesh,
        in_specs=placed,
        out_specs=(P(None, ("kv", "tp")), P("kv", "tp", None, None)),
        check_vma=False,
    )
```
